32 devices in a mesh: grp: 2 (over y), sp: 4 (over z), tp: 4 (over x, core).
Axes of the slice: x: 2, y: 2, z: 4, core: 2. Of those that a mesh axis runs over, the one named last changes fastest.
Arguments:
- latent: bfloat16 [2048, 4096], P(('grp', 'sp')), parts along dimension 0, may hold values from -6 to 6
- context: bfloat16 [512, 4096], P(('grp', 'sp')), parts along dimension 0, may hold values from -6 to 6
- cond_latent: float32 [8192], P(('grp', 'sp')), parts along dimension 0, may hold values from -6 to 6
- cond_context: float32 [8192], P(('grp', 'sp')), parts along dimension 0, may hold values from -6 to 6
- mod_weight: bfloat16 [3, 4096, 4096], P(None, 'sp', 'tp'), may hold values from -0.09375 to 0.09375
- norm_gain: float32 [4096], replicated, may hold values from 0.1 to 1.9
- w_query: bfloat16 [4096, 1024], P('sp', 'tp'), may hold values from -0.09375 to 0.09375
- w_key: bfloat16 [4096, 1024], P('sp', 'tp'), may hold values from -0.09375 to 0.09375
- w_value: bfloat16 [4096, 2048], P('sp', 'tp'), may hold values from -0.09375 to 0.09375
- w_rank: bfloat16 [2, 4096, 64], P(None, 'sp'), may hold values from -0.09375 to 0.09375
- w_decay: bfloat16 [2, 64, 1024], P(None, None, 'tp'), may hold values from -0.75 to 0.75
- decay_bias: float32 [2, 1024], P(None, 'tp'), may hold values from -1 to 20
- decay_shift: float32 [2048, 16], P(('grp', 'sp'), 'tp'), parts along dimension 0, may hold values from -1 to 0
- out_gain: float32 [2048], P('tp'), may hold values from 0.1 to 1.9
- w_out: bfloat16 [2048, 4096], P('tp', 'sp'), may hold values from -0.125 to 0.125
Outputs:
- mixed: bfloat16 [2048, 4096], P(('grp', 'sp')), parts along dimension 0
The draws below stay inside these ranges and needn't reach their ends.
There are 2 independent parts, one for each index of `grp`. The reference program is written for one: setup_inputs(seed, part) draws one part's arguments, and reference() takes and returns one part's arrays. A program takes and returns all parts, laid end to end along the dimension named above; an argument that names none is the same for every part. Nothing has to cross between parts.
All inputs are finite; a program needn't handle non-finite values.
Results may differ from the reference program's by a relative error of at most 0.0095.
Values may be sent and summed in bfloat16 or wider, within the bound.
A program may use at most 128 MiB of HBM per device.

```python
import jax
import jax.numpy as jnp
from jax import lax

D = 4096
HEAD_TOTAL = 16
DK = 64
DV = 128
RANK = 64
BLOCK = 64
L_DEV = 256
CTX = 256
LATENT_TOKENS = 1024
QK = 1024
WIDTH = 2048
GROUPS = 4


def draw_decay_bias(key, part):
    key_mask, key_fast, key_slow = jax.random.split(jax.random.fold_in(key, 11), 3)
    fast_head = jax.random.uniform(key_mask, (2, HEAD_TOTAL)) < 0.5
    fast_values = jax.random.uniform(key_fast, (2, QK), minval=-0.5, maxval=1.0)
    slow_values = jnp.log(LATENT_TOKENS / 4.8) + jax.random.uniform(key_slow, (2, QK), minval=-0.5, maxval=0.5)
    chosen = jnp.repeat(fast_head, DK, axis=1)
    return jnp.where(chosen, fast_values, slow_values).astype(jnp.float32)


def draw_decay_shift(key, part):
    key_speed, key_spike, key_level = jax.random.split(jax.random.fold_in(key, 23), 3)
    segments = LATENT_TOKENS // L_DEV
    rates = jnp.exp(jax.random.uniform(key_speed, (segments, 1, HEAD_TOTAL), minval=jnp.log(0.2), maxval=jnp.log(0.8)))
    baseline = -jnp.broadcast_to(rates, (segments, L_DEV, HEAD_TOTAL)).reshape(LATENT_TOKENS, HEAD_TOTAL) / LATENT_TOKENS
    struck_entries = jax.random.uniform(key_spike, (LATENT_TOKENS, HEAD_TOTAL)) < 2.0 / LATENT_TOKENS
    depths = jnp.log(jax.random.uniform(key_level, (LATENT_TOKENS, HEAD_TOTAL), minval=0.5, maxval=0.8))
    return (baseline + jnp.where(struck_entries, depths, 0.0)).astype(jnp.float32)


def block_levels(own_key, dims, shards, least, top_value):
    def one(dim, parts):
        steps = jax.random.uniform(jax.random.fold_in(jax.random.fold_in(own_key, 6), dim), (parts,), jnp.float32, least / len(shards), top_value / len(shards))
        return jnp.repeat(jnp.exp(steps), dims[dim] // parts).reshape((-1,) + (1,) * (len(dims) - dim - 1))

    loudness = one(*shards[0])
    for cut in shards[1:]:
        loudness = loudness * one(*cut)
    return loudness


def centred(own_key, dims, spread, bound, cuts=(), kind=jnp.bfloat16):
    drawn = spread * jax.random.normal(own_key, dims, jnp.float32)
    if cuts:
        drawn = drawn * block_levels(own_key, dims, cuts, -0.22, 0.18)
    return jnp.clip(drawn, -bound, bound).astype(kind)


def setup_inputs(seed: int = 0, part: int = 0) -> dict:
    arg_keys = jax.random.split(jax.random.key(seed), 16)
    part_splits = jax.random.split(jax.random.fold_in(arg_keys[15], part), 16)
    latent = centred(part_splits[0], (LATENT_TOKENS, D), 1.0, 6.0, ((0, 4),))
    context = centred(part_splits[1], (CTX, D), 1.0, 6.0, ((0, 4),))
    cond_latent = centred(part_splits[2], (D,), 1.0, 6.0, ((0, 4),), jnp.float32)
    cond_context = centred(part_splits[3], (D,), 1.0, 6.0, ((0, 4),), jnp.float32)
    mod_weight = centred(arg_keys[4], (3, D, D), D ** -0.5, 0.09375, ((1, 4), (2, 4)))
    norm_gain = jnp.clip(1.0 + 0.18 * jax.random.normal(arg_keys[5], (D,), jnp.float32), 0.1, 1.9)
    w_query = centred(arg_keys[6], (D, QK), D ** -0.5, 0.09375, ((0, 4), (1, 4)))
    w_key = centred(arg_keys[7], (D, QK), D ** -0.5, 0.09375, ((0, 4), (1, 4)))
    w_value = centred(arg_keys[8], (D, WIDTH), D ** -0.5, 0.09375, ((0, 4), (1, 4)))
    w_rank = centred(arg_keys[9], (2, D, RANK), D ** -0.5, 0.09375, ((1, 4),))
    w_decay = centred(arg_keys[10], (2, RANK, QK), RANK ** -0.5, 0.75, ((2, 4),))
    decay_bias = draw_decay_bias(jax.random.fold_in(arg_keys[15], 71), part)
    decay_shift = draw_decay_shift(jax.random.fold_in(jax.random.fold_in(arg_keys[15], part), 71), part)
    out_gain = jnp.clip(1.0 + 0.18 * jax.random.normal(arg_keys[13], (WIDTH,), jnp.float32), 0.1, 1.9)
    w_out = centred(arg_keys[14], (WIDTH, D), WIDTH ** -0.5, 0.125, ((0, 4), (1, 4)))
    return {"latent": latent, "context": context, "cond_latent": cond_latent, "cond_context": cond_context, "mod_weight": mod_weight, "norm_gain": norm_gain, "w_query": w_query, "w_key": w_key, "w_value": w_value, "w_rank": w_rank, "w_decay": w_decay, "decay_bias": decay_bias, "decay_shift": decay_shift, "out_gain": out_gain, "w_out": w_out}


eps = 1e-06
normalizer = 16.0
precise = lax.Precision.HIGHEST

def rounded(tensor):
    return lax.optimization_barrier(tensor.astype(jnp.bfloat16))

def modulated(tokens, norm_gain, shift_row, scale_row):
    widened = tokens.astype(jnp.float32)
    normalized = widened * lax.rsqrt(lax.optimization_barrier(jnp.mean(widened * widened, axis=-1, keepdims=True)) + eps)
    return (normalized * norm_gain * (1.0 + scale_row) + shift_row).astype(jnp.bfloat16)

def project(tokens, weight):
    return rounded(jnp.dot(tokens, weight, preferred_element_type=jnp.float32))

def log_decay(rank_rows, weight, bias):
    return jax.nn.log_sigmoid(jnp.dot(rank_rows, weight, preferred_element_type=jnp.float32) + bias) / normalizer

def by_heads(tensor, width):
    return tensor.astype(jnp.float32).reshape(tensor.shape[0], -1, width)

def context_state(key_rows, value_rows, decays, forward):
    running = jnp.cumsum(decays, axis=0)
    if forward:
        factor = jnp.exp(running[-1] - running)
    else:
        factor = jnp.exp(running - decays)
    return jnp.einsum('thd,the->hde', key_rows * factor, value_rows, precision=precise)

def chain(queries, key_rows, value_rows, decays, initial):
    length, head_count, _ = queries.shape
    blocks = length // BLOCK
    lower_mask = jnp.tril(jnp.ones((BLOCK, BLOCK), dtype=bool))

    def in_blocks(tensor):
        return tensor.reshape(blocks, BLOCK, head_count, tensor.shape[-1])

    def advance(carry_state, inputs):
        query_block, key_block, value_block, decay_block = inputs
        running = jnp.cumsum(decay_block, axis=0)
        carried = jnp.einsum('chd,hde->che', query_block * jnp.exp(running), carry_state, precision=precise)
        relative = jnp.where(lower_mask[:, :, None, None], running[:, None] - running[None, :], -jnp.inf)
        scores = jnp.einsum('ihd,jhd,ijhd->ijh', query_block, key_block, jnp.exp(relative), precision=precise)
        within = jnp.einsum('ijh,jhe->ihe', scores, value_block, precision=precise)
        block_total = running[-1]
        carry_state = jnp.exp(block_total)[:, :, None] * carry_state + jnp.einsum('chd,che->hde', key_block * jnp.exp(block_total - running), value_block, precision=precise)
        return (carry_state, carried + within)
    _, outputs = lax.scan(advance, initial, (in_blocks(queries), in_blocks(key_rows), in_blocks(value_rows), in_blocks(decays)))
    return outputs.reshape(length, head_count, value_rows.shape[-1])

def reference(latent, context, cond_latent, cond_context, mod_weight, norm_gain, w_query, w_key, w_value, w_rank, w_decay, decay_bias, decay_shift, out_gain, w_out):
    silu_latent = rounded(jax.nn.silu(cond_latent))
    silu_context = rounded(jax.nn.silu(cond_context))
    widened_mod = mod_weight.astype(jnp.float32)
    mod_latent = jnp.einsum('d,rdc->rc', silu_latent.astype(jnp.float32), widened_mod, precision=precise)
    mod_context = jnp.einsum('d,rdc->rc', silu_context.astype(jnp.float32), widened_mod[:2], precision=precise)
    h_latent = modulated(latent, norm_gain, mod_latent[0], mod_latent[1])
    h_context = modulated(context, norm_gain, mod_context[0], mod_context[1])
    queries = by_heads(project(h_latent, w_query), DK)
    key_rows = by_heads(project(h_latent, w_key), DK)
    value_rows = by_heads(project(h_latent, w_value), DV)
    shift_rows = decay_shift[:, :, None]
    log_fwd = by_heads(log_decay(project(h_latent, w_rank[0]), w_decay[0], decay_bias[0]), DK) + shift_rows
    log_bwd = by_heads(log_decay(project(h_latent, w_rank[1]), w_decay[1], decay_bias[1]), DK) + shift_rows
    context_keys = by_heads(project(h_context, w_key), DK)
    context_values = by_heads(project(h_context, w_value), DV)
    context_fwd = by_heads(log_decay(project(h_context, w_rank[0]), w_decay[0], decay_bias[0]), DK)
    context_bwd = by_heads(log_decay(project(h_context, w_rank[1]), w_decay[1], decay_bias[1]), DK)
    start_fwd = context_state(context_keys, context_values, context_fwd, True)
    start_bwd = context_state(context_keys, context_values, context_bwd, False)
    out_fwd = chain(queries, key_rows, value_rows, log_fwd, start_fwd)
    out_bwd = jnp.flip(chain(jnp.flip(queries, 0), jnp.flip(key_rows, 0), jnp.flip(value_rows, 0), jnp.flip(log_bwd, 0), start_bwd), 0)
    combined = out_fwd + out_bwd
    combined = combined * lax.rsqrt(lax.optimization_barrier(jnp.mean(combined * combined, axis=-1, keepdims=True)) + eps)
    normed = (combined.reshape(combined.shape[0], -1) * out_gain).astype(jnp.bfloat16)
    group_width = normed.shape[1] // GROUPS
    summed = jnp.zeros((normed.shape[0], w_out.shape[1]), jnp.float32)
    for group in range(GROUPS):
        lower_edge = group * group_width
        part = rounded(jnp.dot(normed[:, lower_edge:lower_edge + group_width], w_out[lower_edge:lower_edge + group_width], preferred_element_type=jnp.float32))
        summed = summed + part.astype(jnp.float32)
    return (latent.astype(jnp.float32) + mod_latent[2] * summed).astype(jnp.bfloat16)
```

```python
import functools

import jax
import jax.numpy as jnp
from jax import lax
from jax.experimental import pallas as pl
from jax.experimental.pallas import tpu as pltpu
from jax.sharding import PartitionSpec as P

DK = 64
DV = 128
BLOCK = 64


eps = 1e-06
normalizer = 16.0
precise = lax.Precision.HIGHEST


def carried_in(array, axis, join, neutral, backward):
    count = lax.axis_size(axis)
    place = lax.axis_index(axis)
    ahead = count - 1 - place if backward else place
    gathered = jax.tree.map(
        lambda a, kind: lax.all_gather(a.astype(kind), axis),
        array,
        jax.tree.map(lambda a: jnp.bfloat16 if a.dtype == jnp.float32 else a.dtype, array),
    )
    state = jax.tree.map(lambda a, e: jnp.zeros_like(a) + jnp.asarray(e, a.dtype), array, neutral)

    def one(turn, state):
        source = count - 1 - turn if backward else turn
        return join(
            state,
            jax.tree.map(
                lambda a, own: lax.dynamic_index_in_dim(a, source, 0, False).astype(own.dtype),
                gathered,
                array,
            ),
        )

    return lax.fori_loop(0, ahead, one, state)


def rounded(tensor):
    return lax.optimization_barrier(tensor.astype(jnp.bfloat16))


def modulated(tokens, norm_gain, shift_row, scale_row):
    widened = tokens.astype(jnp.float32)
    normalized = widened * lax.rsqrt(jnp.mean(widened * widened, axis=-1, keepdims=True) + eps)
    return (normalized * norm_gain * (1.0 + scale_row) + shift_row).astype(jnp.bfloat16)


def project(tokens, weight):
    return rounded(jnp.dot(tokens, weight, preferred_element_type=jnp.float32))


def log_decay(rank_rows, weight, bias):
    return (
        jax.nn.log_sigmoid(jnp.dot(rank_rows, weight, preferred_element_type=jnp.float32) + bias)
        / normalizer
    )


def by_heads(tensor, width):
    return tensor.astype(jnp.float32).reshape(tensor.shape[0], -1, width)


def context_state(key_rows, value_rows, decays, forward):
    running = jnp.cumsum(decays, axis=0)
    if forward:
        factor = jnp.exp(running[-1] - running)
    else:
        factor = jnp.exp(running - decays)
    return jnp.einsum("thd,the->hde", key_rows * factor, value_rows, precision=precise)


def chained(earlier, later):
    return (earlier[0] + later[0], jnp.exp(later[0])[:, :, None] * earlier[1] + later[1])


def segment_chain(queries, key_rows, value_rows, decays):
    length, head_count, width = queries.shape
    blocks = length // BLOCK
    lower_mask = jnp.tril(jnp.ones((BLOCK, BLOCK), dtype=bool))

    def in_blocks(tensor):
        return tensor.reshape(blocks, BLOCK, head_count, tensor.shape[-1])

    def advance(carry, inputs):
        carry_state, offset = carry
        query_block, key_block, value_block, decay_block = inputs
        running = jnp.cumsum(decay_block, axis=0)
        carried = jnp.einsum(
            "chd,hde->che", query_block * jnp.exp(running), carry_state, precision=precise
        )
        flat_running = running.reshape(BLOCK, head_count * width)
        relative = jnp.where(
            lower_mask[:, :, None], flat_running[:, None] - flat_running[None, :], -jnp.inf
        )
        products = (
            jnp.exp(relative) * query_block.reshape(BLOCK, 1, -1) * key_block.reshape(1, BLOCK, -1)
        )
        scores = products.reshape(BLOCK, BLOCK, head_count, width).sum(axis=-1)
        within = jnp.einsum("ijh,jhe->ihe", scores, value_block, precision=precise)
        block_total = running[-1]
        carry_state = jnp.exp(block_total)[:, :, None] * carry_state + jnp.einsum(
            "chd,che->hde",
            key_block * jnp.exp(block_total - running),
            value_block,
            precision=precise,
        )
        lifted = query_block * jnp.exp(offset + running)
        return ((carry_state, offset + block_total), (carried + within, lifted))

    initial = (
        jnp.zeros((head_count, width, value_rows.shape[-1]), jnp.float32),
        jnp.zeros((head_count, width), jnp.float32),
    )
    (final_state, totals), (outputs, lifted) = lax.scan(
        advance,
        initial,
        (in_blocks(queries), in_blocks(key_rows), in_blocks(value_rows), in_blocks(decays)),
    )
    return (
        outputs.reshape(length, head_count, -1),
        lifted.reshape(length, head_count, width),
        (totals, final_state),
    )


def local(
    latent,
    context,
    cond_latent,
    cond_context,
    mod_weight,
    norm_gain,
    w_query,
    w_key,
    w_value,
    w_rank,
    w_decay,
    decay_bias,
    decay_shift,
    out_gain,
    w_out,
):
    silu_latent = jax.nn.silu(cond_latent).astype(jnp.bfloat16)
    silu_context = jax.nn.silu(cond_context).astype(jnp.bfloat16)
    term_latent = jnp.einsum(
        "d,rdc->rc", silu_latent, mod_weight, preferred_element_type=jnp.float32
    )
    term_context = jnp.einsum(
        "d,rdc->rc", silu_context, mod_weight[:2], preferred_element_type=jnp.float32
    )
    terms = jnp.concatenate([term_latent, term_context], axis=0)
    summed_terms = lax.psum(terms, "sp")
    modulation = lax.all_gather(summed_terms, "tp", axis=1, tiled=True)
    query_all, key_all, value_all, rank_all, output_all, context_rows = (
        lax.all_gather(w_query, "sp", axis=0, tiled=True),
        lax.all_gather(w_key, "sp", axis=0, tiled=True),
        lax.all_gather(w_value, "sp", axis=0, tiled=True),
        lax.all_gather(w_rank, "sp", axis=1, tiled=True),
        lax.all_gather(w_out, "sp", axis=1, tiled=True),
        lax.all_gather(context, "sp", axis=0, tiled=True),
    )
    h_latent = modulated(latent, norm_gain, modulation[0], modulation[1])
    h_context = modulated(context_rows, norm_gain, modulation[3], modulation[4])
    queries = by_heads(project(h_latent, query_all), DK)
    key_rows = by_heads(project(h_latent, key_all), DK)
    value_rows = by_heads(project(h_latent, value_all), DV)
    shift_rows = decay_shift[:, :, None]
    log_fwd = (
        by_heads(log_decay(project(h_latent, rank_all[0]), w_decay[0], decay_bias[0]), DK)
        + shift_rows
    )
    log_bwd = (
        by_heads(log_decay(project(h_latent, rank_all[1]), w_decay[1], decay_bias[1]), DK)
        + shift_rows
    )
    context_keys = by_heads(project(h_context, key_all), DK)
    context_values = by_heads(project(h_context, value_all), DV)
    context_fwd = by_heads(
        log_decay(project(h_context, rank_all[0]), w_decay[0], decay_bias[0]), DK
    )
    context_bwd = by_heads(
        log_decay(project(h_context, rank_all[1]), w_decay[1], decay_bias[1]), DK
    )
    own_fwd = (
        jnp.sum(context_fwd, axis=0),
        context_state(context_keys, context_values, context_fwd, True),
    )
    own_bwd = (
        jnp.sum(context_bwd, axis=0),
        context_state(context_keys, context_values, context_bwd, False),
    )
    out_fwd, lift_fwd, pair_fwd = segment_chain(queries, key_rows, value_rows, log_fwd)
    flipped_out, flipped_lift, pair_bwd = segment_chain(
        jnp.flip(queries, 0), jnp.flip(key_rows, 0), jnp.flip(value_rows, 0), jnp.flip(log_bwd, 0)
    )
    out_bwd = jnp.flip(flipped_out, 0)
    lift_bwd = jnp.flip(flipped_lift, 0)
    zero_pair = (jnp.zeros_like(pair_fwd[0]), jnp.zeros_like(pair_fwd[1]))
    before = carried_in(pair_fwd, "sp", chained, zero_pair, False)
    after = carried_in(pair_bwd, "sp", chained, zero_pair, True)
    start_fwd = own_fwd[1]
    start_bwd = own_bwd[1]
    entry_forward = chained((zero_pair[0], start_fwd), before)[1]
    entry_bwd = chained((zero_pair[0], start_bwd), after)[1]
    combined = (
        out_fwd
        + out_bwd
        + jnp.einsum("thd,hde->the", lift_fwd, entry_forward, precision=precise)
        + jnp.einsum("thd,hde->the", lift_bwd, entry_bwd, precision=precise)
    )
    combined = combined * lax.rsqrt(jnp.mean(combined * combined, axis=-1, keepdims=True) + eps)
    normed = (combined.reshape(combined.shape[0], -1) * out_gain).astype(jnp.bfloat16)
    partial_out = jnp.dot(normed, output_all, preferred_element_type=jnp.float32)
    summed = lax.psum(partial_out.astype(jnp.bfloat16), "tp").astype(jnp.float32)
    return (latent.astype(jnp.float32) + modulation[2] * summed).astype(jnp.bfloat16)


MESH = pl.DeviceIdType.MESH
SUB = 16


def exchange_kernel(axis, count, sends, *refs):
    total = len(sends)
    sources, targets = refs[:total], refs[total : 2 * total]
    send_sem, recv_sem, own_sem = refs[2 * total :]
    me = lax.axis_index(axis)
    barrier = pltpu.get_barrier_semaphore()
    for step in range(1, count):
        pl.semaphore_signal(
            barrier, inc=1, device_id={axis: lax.rem(me + step, count)}, device_id_type=MESH
        )
    pl.semaphore_wait(barrier, count - 1)
    copies = []
    for item in range(total):
        for step in range(1, count):
            peer = lax.rem(me + step, count)
            copy = pltpu.make_async_remote_copy(
                src_ref=sources[item].at[peer] if sends[item] else sources[item],
                dst_ref=targets[item].at[me],
                send_sem=send_sem.at[item, step - 1],
                recv_sem=recv_sem.at[item, step - 1],
                device_id={axis: peer},
                device_id_type=MESH,
            )
            copy.start()
            copies.append(copy)
    for item in range(total):
        copy = pltpu.make_async_copy(
            sources[item].at[me] if sends[item] else sources[item],
            targets[item].at[me],
            own_sem.at[item],
        )
        copy.start()
        copies.append(copy)
    for copy in copies:
        copy.wait()


def exchange(axis, collective, *items):
    count = lax.axis_size(axis)
    sends = tuple(scatter for _, scatter in items)
    arrays = [array for array, _ in items]
    shapes = [
        jax.ShapeDtypeStruct(a.shape if s else (count,) + a.shape, a.dtype) for a, s in items
    ]
    return pl.pallas_call(
        functools.partial(exchange_kernel, axis, count, sends),
        out_shape=shapes,
        in_specs=[pl.BlockSpec(memory_space=pltpu.VMEM)] * len(items),
        out_specs=[pl.BlockSpec(memory_space=pltpu.VMEM)] * len(items),
        scratch_shapes=[
            pltpu.SemaphoreType.DMA((len(items), count - 1)),
            pltpu.SemaphoreType.DMA((len(items), count - 1)),
            pltpu.SemaphoreType.DMA((len(items),)),
        ],
        compiler_params=pltpu.CompilerParams(collective_id=collective, has_side_effects=True),
        name=f"exchange_{collective}",
    )(*arrays)


def narrow_dot(left, right, dims):
    return lax.dot_general(
        left.astype(jnp.bfloat16),
        right.astype(jnp.bfloat16),
        (dims, ((), ())),
        preferred_element_type=jnp.float32,
    )


def mix_kernel(q_ref, k_ref, v_ref, f_ref, b_ref, ck_ref, cv_ref, cf_ref, cb_ref, gain_ref, o_ref, later_ref):
    length, width = q_ref.shape
    depth = v_ref.shape[1]
    row = lax.broadcasted_iota(jnp.int32, (BLOCK, BLOCK), 0)
    column = lax.broadcasted_iota(jnp.int32, (BLOCK, BLOCK), 1)
    lower = jnp.where(row >= column, 1.0, 0.0).astype(jnp.float32)
    upper = jnp.where(row <= column, 1.0, 0.0).astype(jnp.float32)
    key_row = lax.broadcasted_iota(jnp.int32, (BLOCK, width), 0)

    def sums(ones, decays):
        return jnp.dot(ones, decays, precision=precise, preferred_element_type=jnp.float32)

    def step(state, keys, values, running, block_total):
        return state * jnp.exp(block_total) + narrow_dot(
            values, keys * jnp.exp(block_total - running), ((0,), (0,))
        )

    def at(ref, index):
        return ref[pl.ds(pl.multiple_of(index * BLOCK, BLOCK), BLOCK), :].astype(jnp.float32)

    zero = jnp.zeros((depth, width), jnp.float32)
    context_blocks = ck_ref.shape[0] // BLOCK
    blocks = length // BLOCK

    def context_forward(index, state):
        running = sums(lower, at(cf_ref, index))
        return step(state, at(ck_ref, index), at(cv_ref, index), running, running[BLOCK - 1 :])

    def context_backward(turn, state):
        index = context_blocks - 1 - turn
        running = sums(upper, at(cb_ref, index))
        return step(state, at(ck_ref, index), at(cv_ref, index), running, running[:1])

    start_fwd = lax.fori_loop(0, context_blocks, context_forward, zero)
    start_bwd = lax.fori_loop(0, context_blocks, context_backward, zero)

    def backward(turn, state):
        index = blocks - 1 - turn
        later_ref[index] = state
        running = sums(upper, at(b_ref, index))
        return step(state, at(k_ref, index), at(v_ref, index), running, running[:1])

    lax.fori_loop(0, blocks, backward, start_bwd)

    def forward(index, state):
        queries, keys, values = at(q_ref, index), at(k_ref, index), at(v_ref, index)
        ahead = sums(lower, at(f_ref, index))
        behind = sums(upper, at(b_ref, index))
        pieces = []
        for sub in range(BLOCK // SUB):
            low, high = sub * SUB, (sub + 1) * SUB
            own = slice(low, high)
            left, right = [], []
            if low:
                edge = ahead[low - 1 : low]
                left.append(queries[own] * jnp.exp(ahead[own] - edge))
                right.append(
                    jnp.where(key_row < low, keys * jnp.exp(jnp.minimum(edge - ahead, 0.0)), 0.0)
                )
            if high < BLOCK:
                edge = behind[high : high + 1]
                left.append(queries[own] * jnp.exp(behind[own] - edge))
                right.append(
                    jnp.where(key_row >= high, keys * jnp.exp(jnp.minimum(edge - behind, 0.0)), 0.0)
                )
            piece = narrow_dot(left[0], right[0], ((1,), (1,)))
            for one, other in zip(left[1:], right[1:]):
                piece = piece + narrow_dot(one, other, ((1,), (1,)))
            pieces.append(piece)
        scores = jnp.concatenate(pieces, axis=0)

        def cut(tensor):
            return tensor.reshape(BLOCK // SUB, SUB, width)

        q3, k3, a3, b3 = cut(queries), cut(keys), cut(ahead), cut(behind)
        inner = lax.broadcasted_iota(jnp.int32, q3.shape, 1)
        for other in range(SUB):
            one = slice(other, other + 1)
            relative = jnp.where(inner >= other, a3 - a3[:, one], b3 - b3[:, one])
            product = jnp.exp(relative) * q3 * k3[:, one]
            product = jnp.where(inner == other, 2.0 * product, product)
            near = jnp.sum(product.reshape(BLOCK, width), axis=-1, keepdims=True)
            scores = scores + jnp.where(column == (row // SUB) * SUB + other, near, 0.0)
        output = (
            narrow_dot(scores, values, ((1,), (0,)))
            + narrow_dot(queries * jnp.exp(ahead), state, ((1,), (1,)))
            + narrow_dot(queries * jnp.exp(behind), later_ref[index], ((1,), (1,)))
        )
        output = output * lax.rsqrt(jnp.mean(output * output, axis=-1, keepdims=True) + eps)
        o_ref[pl.ds(pl.multiple_of(index * BLOCK, BLOCK), BLOCK), :] = (
            output * gain_ref[...]
        ).astype(o_ref.dtype)
        return step(state, keys, values, ahead, ahead[BLOCK - 1 :])

    lax.fori_loop(0, blocks, forward, start_fwd)


def mix(queries, key_rows, value_rows, log_fwd, log_bwd, keys, values, fwd, bwd, gain):
    length, width = queries.shape
    depth = value_rows.shape[1]
    return pl.pallas_call(
        mix_kernel,
        out_shape=jax.ShapeDtypeStruct((length, depth), jnp.bfloat16),
        in_specs=[pl.BlockSpec(memory_space=pltpu.VMEM)] * 10,
        out_specs=pl.BlockSpec(memory_space=pltpu.VMEM),
        scratch_shapes=[pltpu.VMEM((length // BLOCK, depth, width), jnp.float32)],
        name="mix",
    )(queries, key_rows, value_rows, log_fwd, log_bwd, keys, values, fwd, bwd, gain)


def local_heads(
    latent,
    context,
    cond_latent,
    cond_context,
    mod_weight,
    norm_gain,
    w_query,
    w_key,
    w_value,
    w_rank,
    w_decay,
    decay_bias,
    decay_shift,
    out_gain,
    w_out,
):
    sp, tp = lax.axis_size("sp"), lax.axis_size("tp")
    at_sp, at_tp = lax.axis_index("sp"), lax.axis_index("tp")
    rows, model = latent.shape
    context_rows = context.shape[0]
    inner = model // sp
    heads = w_query.shape[1] // DK
    silu_latent = jax.nn.silu(cond_latent).astype(jnp.bfloat16)
    silu_context = jax.nn.silu(cond_context).astype(jnp.bfloat16)
    term_latent = jnp.einsum(
        "d,rdc->rc", silu_latent, mod_weight, preferred_element_type=jnp.float32
    )
    term_context = jnp.einsum(
        "d,rdc->rc", silu_context, mod_weight[:2], preferred_element_type=jnp.float32
    )
    terms = jnp.concatenate([term_latent, term_context], axis=0)

    def inverse(tokens):
        widened = tokens.astype(jnp.float32)
        return lax.rsqrt(jnp.mean(widened * widened, axis=-1) + eps)

    scales = jnp.concatenate([inverse(latent), inverse(context)])[None]

    def share(tokens):
        quarter = tokens.shape[0] // tp
        own = lax.dynamic_slice_in_dim(tokens, at_tp * quarter, quarter, 0)
        return own.reshape(quarter, sp, inner).transpose(1, 0, 2)

    latent_share, context_share, terms_all, scales_all, shift_all = exchange(
        "sp",
        1,
        (share(latent), True),
        (share(context), True),
        (terms, False),
        (scales, False),
        (decay_shift.T[:, None, :], True),
    )
    latent_all, context_all, modulation = exchange(
        "tp",
        2,
        (latent_share, False),
        (context_share, False),
        (jnp.sum(terms_all, axis=0), False),
    )
    modulation = modulation.transpose(1, 0, 2).reshape(terms.shape[0], model)
    own_mod = lax.dynamic_slice_in_dim(modulation, at_sp * inner, inner, 1)
    own_gain = lax.dynamic_slice_in_dim(norm_gain, at_sp * inner, inner, 0)
    raw_latent = latent_all.transpose(1, 0, 2, 3).reshape(sp * rows, inner)
    raw_context = context_all.transpose(1, 0, 2, 3).reshape(sp * context_rows, inner)

    def tokens_of(raw, inverses, shift_row, scale_row):
        normalized = raw.astype(jnp.float32) * inverses.reshape(-1, 1)
        return (normalized * own_gain * (1.0 + scale_row) + shift_row).astype(jnp.bfloat16)

    h_latent = tokens_of(raw_latent, scales_all[:, 0, :rows], own_mod[0], own_mod[1])
    h_context = tokens_of(raw_context, scales_all[:, 0, rows:], own_mod[3], own_mod[4])
    h_all = jnp.concatenate([h_latent, h_context], axis=0)
    weights = jnp.concatenate(
        [
            w_query.reshape(inner, heads, DK),
            w_key.reshape(inner, heads, DK),
            w_value.reshape(inner, heads, DV),
        ],
        axis=2,
    ).transpose(1, 0, 2)
    partial = jnp.einsum(
        "tk,hkc->htc", h_all, weights, preferred_element_type=jnp.float32
    ).astype(jnp.bfloat16)

    def my_rows(tokens):
        cut = tokens.reshape(sp, tp, -1, inner)
        return lax.dynamic_index_in_dim(cut, at_tp, 1, False).reshape(-1, inner)

    rank_rows = jnp.concatenate([my_rows(h_latent), my_rows(h_context)], axis=0)
    rank_partial = jnp.dot(
        rank_rows,
        jnp.concatenate([w_rank[0], w_rank[1]], axis=1),
        preferred_element_type=jnp.float32,
    ).astype(jnp.bfloat16)
    partial_all, rank_all = exchange("sp", 3, (partial, True), (rank_partial, False))
    rank_own = jnp.sum(rank_all.astype(jnp.float32), axis=0).astype(jnp.bfloat16)
    (rank_full,) = exchange("tp", 4, (rank_own, False))
    width = rank_full.shape[-1]
    cut = rank_rows.shape[0] - sp * context_rows // tp

    def in_order(tensor):
        return tensor.reshape(tp, sp, -1, width).transpose(1, 0, 2, 3).reshape(-1, width)

    ranks = jnp.concatenate([in_order(rank_full[:, :cut]), in_order(rank_full[:, cut:])], axis=0)
    joined = jnp.sum(partial_all.astype(jnp.float32), axis=0).astype(jnp.bfloat16)
    own_decay = lax.dynamic_slice_in_dim(w_decay, at_sp * DK, DK, 2)
    own_bias = lax.dynamic_slice_in_dim(decay_bias, at_sp * DK, DK, 1)
    half = width // 2
    fwd = log_decay(ranks[:, :half], own_decay[0], own_bias[0])
    bwd = log_decay(ranks[:, half:], own_decay[1], own_bias[1])
    span = sp * rows
    shift_rows = shift_all.reshape(span, 1)
    normed = mix(
        joined[:span, :DK],
        joined[:span, DK : 2 * DK],
        joined[:span, 2 * DK :],
        fwd[:span] + shift_rows,
        bwd[:span] + shift_rows,
        joined[span:, DK : 2 * DK],
        joined[span:, 2 * DK :],
        fwd[span:],
        bwd[span:],
        lax.dynamic_slice_in_dim(out_gain, at_sp * DV, DV, 0)[None],
    )
    (normed_all,) = exchange("sp", 5, (normed, False))
    part = jnp.einsum(
        "htc,hcd->td",
        normed_all,
        w_out.reshape(heads, DV, -1),
        preferred_element_type=jnp.float32,
    ).astype(jnp.bfloat16)
    columns = part.shape[1] // tp
    (part_all,) = exchange(
        "tp", 6, (part.reshape(span, tp, columns).transpose(1, 0, 2), True)
    )
    summed = jnp.sum(part_all.astype(jnp.float32), axis=0)
    gate = lax.dynamic_slice_in_dim(own_mod[2], at_tp * columns, columns, 0)
    residual = lax.dynamic_slice_in_dim(raw_latent, at_tp * columns, columns, 1)
    slab = (residual.astype(jnp.float32) + gate * summed).astype(jnp.bfloat16)
    (slab_rows,) = exchange("sp", 7, (slab.reshape(sp, rows, columns), True))
    (slab_all,) = exchange("tp", 8, (slab_rows, False))
    return slab_all.transpose(2, 1, 0, 3).reshape(rows, model)


def chosen(mesh, *arrays):
    sizes = dict(mesh.shape)
    heads = arrays[6].shape[1]
    one_head_each = heads == DK * sizes["sp"] * sizes["tp"]
    return local_heads if one_head_each else local


def solution(mesh):
    return lambda *arrays: jax.shard_map(
        chosen(mesh, *arrays),
        mesh=mesh,
        in_specs=(
            P(("grp", "sp"), None),
            P(("grp", "sp"), None),
            P(("grp", "sp")),
            P(("grp", "sp")),
            P(None, "sp", "tp"),
            P(),
            P("sp", "tp"),
            P("sp", "tp"),
            P("sp", "tp"),
            P(None, "sp", None),
            P(None, None, "tp"),
            P(None, "tp"),
            P(("grp", "sp"), "tp"),
            P("tp"),
            P("tp", "sp"),
        ),
        out_specs=P(("grp", "sp"), None),
        check_vma=False,
    )(*arrays)
```

```python
import functools

import jax
import jax.numpy as jnp
from jax import lax
from jax.experimental import pallas as pl
from jax.experimental.pallas import tpu as pltpu
from jax.sharding import PartitionSpec as P

DK = 64
DV = 128
BLOCK = 64


eps = 1e-06
normalizer = 16.0
precise = lax.Precision.HIGHEST


def carried_in(array, axis, join, neutral, backward):
    count = lax.axis_size(axis)
    place = lax.axis_index(axis)
    ahead = count - 1 - place if backward else place
    gathered = jax.tree.map(
        lambda a, kind: lax.all_gather(a.astype(kind), axis),
        array,
        jax.tree.map(lambda a: jnp.bfloat16 if a.dtype == jnp.float32 else a.dtype, array),
    )
    state = jax.tree.map(lambda a, e: jnp.zeros_like(a) + jnp.asarray(e, a.dtype), array, neutral)

    def one(turn, state):
        source = count - 1 - turn if backward else turn
        return join(
            state,
            jax.tree.map(
                lambda a, own: lax.dynamic_index_in_dim(a, source, 0, False).astype(own.dtype),
                gathered,
                array,
            ),
        )

    return lax.fori_loop(0, ahead, one, state)


def rounded(tensor):
    return lax.optimization_barrier(tensor.astype(jnp.bfloat16))


def modulated(tokens, norm_gain, shift_row, scale_row):
    widened = tokens.astype(jnp.float32)
    normalized = widened * lax.rsqrt(jnp.mean(widened * widened, axis=-1, keepdims=True) + eps)
    return (normalized * norm_gain * (1.0 + scale_row) + shift_row).astype(jnp.bfloat16)


def project(tokens, weight):
    return rounded(jnp.dot(tokens, weight, preferred_element_type=jnp.float32))


def log_decay(rank_rows, weight, bias):
    return (
        jax.nn.log_sigmoid(jnp.dot(rank_rows, weight, preferred_element_type=jnp.float32) + bias)
        / normalizer
    )


def by_heads(tensor, width):
    return tensor.astype(jnp.float32).reshape(tensor.shape[0], -1, width)


def context_state(key_rows, value_rows, decays, forward):
    running = jnp.cumsum(decays, axis=0)
    if forward:
        factor = jnp.exp(running[-1] - running)
    else:
        factor = jnp.exp(running - decays)
    return jnp.einsum("thd,the->hde", key_rows * factor, value_rows, precision=precise)


def chained(earlier, later):
    return (earlier[0] + later[0], jnp.exp(later[0])[:, :, None] * earlier[1] + later[1])


def segment_chain(queries, key_rows, value_rows, decays):
    length, head_count, width = queries.shape
    blocks = length // BLOCK
    lower_mask = jnp.tril(jnp.ones((BLOCK, BLOCK), dtype=bool))

    def in_blocks(tensor):
        return tensor.reshape(blocks, BLOCK, head_count, tensor.shape[-1])

    def advance(carry, inputs):
        carry_state, offset = carry
        query_block, key_block, value_block, decay_block = inputs
        running = jnp.cumsum(decay_block, axis=0)
        carried = jnp.einsum(
            "chd,hde->che", query_block * jnp.exp(running), carry_state, precision=precise
        )
        flat_running = running.reshape(BLOCK, head_count * width)
        relative = jnp.where(
            lower_mask[:, :, None], flat_running[:, None] - flat_running[None, :], -jnp.inf
        )
        products = (
            jnp.exp(relative) * query_block.reshape(BLOCK, 1, -1) * key_block.reshape(1, BLOCK, -1)
        )
        scores = products.reshape(BLOCK, BLOCK, head_count, width).sum(axis=-1)
        within = jnp.einsum("ijh,jhe->ihe", scores, value_block, precision=precise)
        block_total = running[-1]
        carry_state = jnp.exp(block_total)[:, :, None] * carry_state + jnp.einsum(
            "chd,che->hde",
            key_block * jnp.exp(block_total - running),
            value_block,
            precision=precise,
        )
        lifted = query_block * jnp.exp(offset + running)
        return ((carry_state, offset + block_total), (carried + within, lifted))

    initial = (
        jnp.zeros((head_count, width, value_rows.shape[-1]), jnp.float32),
        jnp.zeros((head_count, width), jnp.float32),
    )
    (final_state, totals), (outputs, lifted) = lax.scan(
        advance,
        initial,
        (in_blocks(queries), in_blocks(key_rows), in_blocks(value_rows), in_blocks(decays)),
    )
    return (
        outputs.reshape(length, head_count, -1),
        lifted.reshape(length, head_count, width),
        (totals, final_state),
    )


def local(
    latent,
    context,
    cond_latent,
    cond_context,
    mod_weight,
    norm_gain,
    w_query,
    w_key,
    w_value,
    w_rank,
    w_decay,
    decay_bias,
    decay_shift,
    out_gain,
    w_out,
):
    silu_latent = jax.nn.silu(cond_latent).astype(jnp.bfloat16)
    silu_context = jax.nn.silu(cond_context).astype(jnp.bfloat16)
    term_latent = jnp.einsum(
        "d,rdc->rc", silu_latent, mod_weight, preferred_element_type=jnp.float32
    )
    term_context = jnp.einsum(
        "d,rdc->rc", silu_context, mod_weight[:2], preferred_element_type=jnp.float32
    )
    terms = jnp.concatenate([term_latent, term_context], axis=0)
    summed_terms = lax.psum(terms, "sp")
    modulation = lax.all_gather(summed_terms, "tp", axis=1, tiled=True)
    query_all, key_all, value_all, rank_all, output_all, context_rows = (
        lax.all_gather(w_query, "sp", axis=0, tiled=True),
        lax.all_gather(w_key, "sp", axis=0, tiled=True),
        lax.all_gather(w_value, "sp", axis=0, tiled=True),
        lax.all_gather(w_rank, "sp", axis=1, tiled=True),
        lax.all_gather(w_out, "sp", axis=1, tiled=True),
        lax.all_gather(context, "sp", axis=0, tiled=True),
    )
    h_latent = modulated(latent, norm_gain, modulation[0], modulation[1])
    h_context = modulated(context_rows, norm_gain, modulation[3], modulation[4])
    queries = by_heads(project(h_latent, query_all), DK)
    key_rows = by_heads(project(h_latent, key_all), DK)
    value_rows = by_heads(project(h_latent, value_all), DV)
    shift_rows = decay_shift[:, :, None]
    log_fwd = (
        by_heads(log_decay(project(h_latent, rank_all[0]), w_decay[0], decay_bias[0]), DK)
        + shift_rows
    )
    log_bwd = (
        by_heads(log_decay(project(h_latent, rank_all[1]), w_decay[1], decay_bias[1]), DK)
        + shift_rows
    )
    context_keys = by_heads(project(h_context, key_all), DK)
    context_values = by_heads(project(h_context, value_all), DV)
    context_fwd = by_heads(
        log_decay(project(h_context, rank_all[0]), w_decay[0], decay_bias[0]), DK
    )
    context_bwd = by_heads(
        log_decay(project(h_context, rank_all[1]), w_decay[1], decay_bias[1]), DK
    )
    own_fwd = (
        jnp.sum(context_fwd, axis=0),
        context_state(context_keys, context_values, context_fwd, True),
    )
    own_bwd = (
        jnp.sum(context_bwd, axis=0),
        context_state(context_keys, context_values, context_bwd, False),
    )
    out_fwd, lift_fwd, pair_fwd = segment_chain(queries, key_rows, value_rows, log_fwd)
    flipped_out, flipped_lift, pair_bwd = segment_chain(
        jnp.flip(queries, 0), jnp.flip(key_rows, 0), jnp.flip(value_rows, 0), jnp.flip(log_bwd, 0)
    )
    out_bwd = jnp.flip(flipped_out, 0)
    lift_bwd = jnp.flip(flipped_lift, 0)
    zero_pair = (jnp.zeros_like(pair_fwd[0]), jnp.zeros_like(pair_fwd[1]))
    before = carried_in(pair_fwd, "sp", chained, zero_pair, False)
    after = carried_in(pair_bwd, "sp", chained, zero_pair, True)
    start_fwd = own_fwd[1]
    start_bwd = own_bwd[1]
    entry_forward = chained((zero_pair[0], start_fwd), before)[1]
    entry_bwd = chained((zero_pair[0], start_bwd), after)[1]
    combined = (
        out_fwd
        + out_bwd
        + jnp.einsum("thd,hde->the", lift_fwd, entry_forward, precision=precise)
        + jnp.einsum("thd,hde->the", lift_bwd, entry_bwd, precision=precise)
    )
    combined = combined * lax.rsqrt(jnp.mean(combined * combined, axis=-1, keepdims=True) + eps)
    normed = (combined.reshape(combined.shape[0], -1) * out_gain).astype(jnp.bfloat16)
    partial_out = jnp.dot(normed, output_all, preferred_element_type=jnp.float32)
    summed = lax.psum(partial_out.astype(jnp.bfloat16), "tp").astype(jnp.float32)
    return (latent.astype(jnp.float32) + modulation[2] * summed).astype(jnp.bfloat16)


MESH = pl.DeviceIdType.MESH
SUB = 16


def exchange_kernel(axis, count, sends, *refs):
    total = len(sends)
    sources, targets = refs[:total], refs[total : 2 * total]
    send_sem, recv_sem, own_sem = refs[2 * total :]
    me = lax.axis_index(axis)
    barrier = pltpu.get_barrier_semaphore()
    for step in range(1, count):
        pl.semaphore_signal(
            barrier, inc=1, device_id={axis: lax.rem(me + step, count)}, device_id_type=MESH
        )
    pl.semaphore_wait(barrier, count - 1)
    copies = []
    for item in range(total):
        for step in range(1, count):
            peer = lax.rem(me + step, count)
            copy = pltpu.make_async_remote_copy(
                src_ref=sources[item].at[peer] if sends[item] else sources[item],
                dst_ref=targets[item].at[me],
                send_sem=send_sem.at[item, step - 1],
                recv_sem=recv_sem.at[item, step - 1],
                device_id={axis: peer},
                device_id_type=MESH,
            )
            copy.start()
            copies.append(copy)
    for item in range(total):
        copy = pltpu.make_async_copy(
            sources[item].at[me] if sends[item] else sources[item],
            targets[item].at[me],
            own_sem.at[item],
        )
        copy.start()
        copies.append(copy)
    for copy in copies:
        copy.wait()


def exchange(axis, collective, *items):
    count = lax.axis_size(axis)
    sends = tuple(scatter for _, scatter in items)
    arrays = [array for array, _ in items]
    shapes = [
        jax.ShapeDtypeStruct(a.shape if s else (count,) + a.shape, a.dtype) for a, s in items
    ]
    return pl.pallas_call(
        functools.partial(exchange_kernel, axis, count, sends),
        out_shape=shapes,
        in_specs=[pl.BlockSpec(memory_space=pltpu.VMEM)] * len(items),
        out_specs=[pl.BlockSpec(memory_space=pltpu.VMEM)] * len(items),
        scratch_shapes=[
            pltpu.SemaphoreType.DMA((len(items), count - 1)),
            pltpu.SemaphoreType.DMA((len(items), count - 1)),
            pltpu.SemaphoreType.DMA((len(items),)),
        ],
        compiler_params=pltpu.CompilerParams(collective_id=collective, has_side_effects=True),
        name=f"exchange_{collective}",
    )(*arrays)


def relay_kernel(across, along, items, *refs):
    total = len(items)
    sources, targets = refs[:total], refs[total : 2 * total]
    own_sem, far_send, far_recv, near_send, near_recv, pass_send, pass_recv = refs[2 * total :]
    far, near = lax.axis_size(across), lax.axis_size(along)
    here, mine = lax.axis_index(across), lax.axis_index(along)
    pairs = near // 2
    partner = mine + 1 - 2 * lax.rem(mine, 2)
    barrier = pltpu.get_barrier_semaphore()
    for step in range(1, far):
        pl.semaphore_signal(
            barrier, inc=1, device_id={across: lax.rem(here + step, far)}, device_id_type=MESH
        )
    pl.semaphore_signal(barrier, inc=1, device_id={along: partner}, device_id_type=MESH)
    for step in range(1, pairs):
        pl.semaphore_signal(
            barrier, inc=1, device_id={along: lax.rem(mine + 2 * step, near)}, device_id_type=MESH
        )
    pl.semaphore_wait(barrier, far - 1 + pairs)

    def view(item, source, holder):
        scatter, forward, block = items[item]
        target = targets[item]
        if not forward:
            return target.at[source]
        if block is None:
            return target.at[source, holder]
        start = pl.multiple_of((source * near + holder) * block, block)
        return target.at[:, pl.ds(start, block)]

    def taken(item, peer):
        return sources[item].at[peer] if items[item][0] else sources[item]

    first, sent, arrive = {}, [], []
    for item in range(total):
        copy = pltpu.make_async_copy(taken(item, here), view(item, here, mine), own_sem.at[item])
        copy.start()
        first[item, 0] = copy
        for step in range(1, far):
            peer = lax.rem(here + step, far)
            copy = pltpu.make_async_remote_copy(
                src_ref=taken(item, peer),
                dst_ref=view(item, here, mine),
                send_sem=far_send.at[item, step],
                recv_sem=far_recv.at[item, step],
                device_id={across: peer},
                device_id_type=MESH,
            )
            copy.start()
            first[item, step] = copy
            sent.append(copy)

    def hand(item, step, block, slot, sends, recvs, peer):
        copy = pltpu.make_async_remote_copy(
            src_ref=block,
            dst_ref=block,
            send_sem=sends.at[item, step, slot],
            recv_sem=recvs.at[item, step, slot],
            device_id={along: peer},
            device_id_type=MESH,
        )
        copy.start()
        sent.append(copy)
        return copy

    crossed = []

    def pass_on():
        for item, step, source, slot, copy in crossed:
            copy.wait_recv()
            holder = lax.rem(mine + near - 2 * slot, near)
            block = view(item, source, holder)
            arrive.append(hand(item, step, block, slot, pass_send, pass_recv, partner))
        crossed.clear()

    for step in range(far):
        source = lax.rem(here - step + far, far)
        fresh = []
        for item in range(total):
            if not items[item][1]:
                continue
            if step:
                first[item, step].wait_recv()
            else:
                first[item, step].wait()
            block = view(item, source, mine)
            for slot in range(1, pairs):
                peer = lax.rem(mine + 2 * slot, near)
                copy = hand(item, step, block, slot, near_send, near_recv, peer)
                fresh.append((item, step, source, slot, copy))
            arrive.append(hand(item, step, block, 0, near_send, near_recv, partner))
        pass_on()
        crossed.extend(fresh)
    pass_on()
    for item in range(total):
        if not items[item][1]:
            first[item, 0].wait()
            for step in range(1, far):
                first[item, step].wait_recv()
    for copy in arrive:
        copy.wait_recv()
    for copy in sent:
        copy.wait_send()


def relay(across, along, collective, *items):
    far, near = lax.axis_size(across), lax.axis_size(along)
    shapes = []
    for array, scatter, forward, block in items:
        shape = array.shape[1:] if scatter else array.shape
        if block is not None:
            full = (shape[0], far * near * block)
        elif forward:
            full = (far, near) + shape
        else:
            full = (far,) + shape
        shapes.append(jax.ShapeDtypeStruct(full, array.dtype))
    dma = pltpu.SemaphoreType.DMA
    count, pairs = len(items), near // 2
    return pl.pallas_call(
        functools.partial(relay_kernel, across, along, tuple(i[1:] for i in items)),
        out_shape=shapes,
        in_specs=[pl.BlockSpec(memory_space=pltpu.VMEM)] * count,
        out_specs=[pl.BlockSpec(memory_space=pltpu.VMEM)] * count,
        scratch_shapes=[dma((count,)), dma((count, far)), dma((count, far))]
        + [dma((count, far, pairs))] * 4,
        compiler_params=pltpu.CompilerParams(collective_id=collective, has_side_effects=True),
        name=f"relay_{collective}",
    )(*[item[0] for item in items])


def narrow_dot(left, right, dims):
    return lax.dot_general(
        left.astype(jnp.bfloat16),
        right.astype(jnp.bfloat16),
        (dims, ((), ())),
        preferred_element_type=jnp.float32,
    )


def mix_kernel(q_ref, k_ref, v_ref, f_ref, b_ref, ck_ref, cv_ref, cf_ref, cb_ref, gain_ref, o_ref, later_ref):
    length, width = q_ref.shape
    depth = v_ref.shape[1]
    row = lax.broadcasted_iota(jnp.int32, (BLOCK, BLOCK), 0)
    column = lax.broadcasted_iota(jnp.int32, (BLOCK, BLOCK), 1)
    lower = jnp.where(row >= column, 1.0, 0.0).astype(jnp.float32)
    upper = jnp.where(row <= column, 1.0, 0.0).astype(jnp.float32)
    key_row = lax.broadcasted_iota(jnp.int32, (BLOCK, width), 0)

    def sums(ones, decays):
        return jnp.dot(ones, decays, precision=precise, preferred_element_type=jnp.float32)

    def step(state, keys, values, running, block_total):
        return state * jnp.exp(block_total) + narrow_dot(
            values, keys * jnp.exp(block_total - running), ((0,), (0,))
        )

    def at(ref, index):
        return ref[pl.ds(pl.multiple_of(index * BLOCK, BLOCK), BLOCK), :].astype(jnp.float32)

    zero = jnp.zeros((depth, width), jnp.float32)
    context_blocks = ck_ref.shape[0] // BLOCK
    blocks = length // BLOCK

    def context_forward(index, state):
        running = sums(lower, at(cf_ref, index))
        return step(state, at(ck_ref, index), at(cv_ref, index), running, running[BLOCK - 1 :])

    def context_backward(turn, state):
        index = context_blocks - 1 - turn
        running = sums(upper, at(cb_ref, index))
        return step(state, at(ck_ref, index), at(cv_ref, index), running, running[:1])

    start_fwd = lax.fori_loop(0, context_blocks, context_forward, zero)
    start_bwd = lax.fori_loop(0, context_blocks, context_backward, zero)

    def backward(turn, state):
        index = blocks - 1 - turn
        later_ref[index] = state
        running = sums(upper, at(b_ref, index))
        return step(state, at(k_ref, index), at(v_ref, index), running, running[:1])

    lax.fori_loop(0, blocks, backward, start_bwd)

    def forward(index, state):
        queries, keys, values = at(q_ref, index), at(k_ref, index), at(v_ref, index)
        ahead = sums(lower, at(f_ref, index))
        behind = sums(upper, at(b_ref, index))
        pieces = []
        for sub in range(BLOCK // SUB):
            low, high = sub * SUB, (sub + 1) * SUB
            own = slice(low, high)
            left, right = [], []
            if low:
                edge = ahead[low - 1 : low]
                left.append(queries[own] * jnp.exp(ahead[own] - edge))
                right.append(
                    jnp.where(key_row < low, keys * jnp.exp(jnp.minimum(edge - ahead, 0.0)), 0.0)
                )
            if high < BLOCK:
                edge = behind[high : high + 1]
                left.append(queries[own] * jnp.exp(behind[own] - edge))
                right.append(
                    jnp.where(key_row >= high, keys * jnp.exp(jnp.minimum(edge - behind, 0.0)), 0.0)
                )
            piece = narrow_dot(left[0], right[0], ((1,), (1,)))
            for one, other in zip(left[1:], right[1:]):
                piece = piece + narrow_dot(one, other, ((1,), (1,)))
            pieces.append(piece)
        scores = jnp.concatenate(pieces, axis=0)

        def cut(tensor):
            return tensor.reshape(BLOCK // SUB, SUB, width)

        q3, k3, a3, b3 = cut(queries), cut(keys), cut(ahead), cut(behind)
        inner = lax.broadcasted_iota(jnp.int32, q3.shape, 1)
        for other in range(SUB):
            one = slice(other, other + 1)
            relative = jnp.where(inner >= other, a3 - a3[:, one], b3 - b3[:, one])
            product = jnp.exp(relative) * q3 * k3[:, one]
            product = jnp.where(inner == other, 2.0 * product, product)
            near = jnp.sum(product.reshape(BLOCK, width), axis=-1, keepdims=True)
            scores = scores + jnp.where(column == (row // SUB) * SUB + other, near, 0.0)
        output = (
            narrow_dot(scores, values, ((1,), (0,)))
            + narrow_dot(queries * jnp.exp(ahead), state, ((1,), (1,)))
            + narrow_dot(queries * jnp.exp(behind), later_ref[index], ((1,), (1,)))
        )
        output = output * lax.rsqrt(jnp.mean(output * output, axis=-1, keepdims=True) + eps)
        o_ref[pl.ds(pl.multiple_of(index * BLOCK, BLOCK), BLOCK), :] = (
            output * gain_ref[...]
        ).astype(o_ref.dtype)
        return step(state, keys, values, ahead, ahead[BLOCK - 1 :])

    lax.fori_loop(0, blocks, forward, start_fwd)


def mix(queries, key_rows, value_rows, log_fwd, log_bwd, keys, values, fwd, bwd, gain):
    length, width = queries.shape
    depth = value_rows.shape[1]
    return pl.pallas_call(
        mix_kernel,
        out_shape=jax.ShapeDtypeStruct((length, depth), jnp.bfloat16),
        in_specs=[pl.BlockSpec(memory_space=pltpu.VMEM)] * 10,
        out_specs=pl.BlockSpec(memory_space=pltpu.VMEM),
        scratch_shapes=[pltpu.VMEM((length // BLOCK, depth, width), jnp.float32)],
        name="mix",
    )(queries, key_rows, value_rows, log_fwd, log_bwd, keys, values, fwd, bwd, gain)


def local_heads(
    latent,
    context,
    cond_latent,
    cond_context,
    mod_weight,
    norm_gain,
    w_query,
    w_key,
    w_value,
    w_rank,
    w_decay,
    decay_bias,
    decay_shift,
    out_gain,
    w_out,
):
    sp, tp = lax.axis_size("sp"), lax.axis_size("tp")
    at_sp, at_tp = lax.axis_index("sp"), lax.axis_index("tp")
    rows, model = latent.shape
    context_rows = context.shape[0]
    inner = model // sp
    heads = w_query.shape[1] // DK
    silu_latent = jax.nn.silu(cond_latent).astype(jnp.bfloat16)
    silu_context = jax.nn.silu(cond_context).astype(jnp.bfloat16)
    term_latent = jnp.einsum(
        "d,rdc->rc", silu_latent, mod_weight, preferred_element_type=jnp.float32
    )
    term_context = jnp.einsum(
        "d,rdc->rc", silu_context, mod_weight[:2], preferred_element_type=jnp.float32
    )
    terms = jnp.concatenate([term_latent, term_context], axis=0)

    def inverse(tokens):
        widened = tokens.astype(jnp.float32)
        return lax.rsqrt(jnp.mean(widened * widened, axis=-1) + eps)

    scales = jnp.concatenate([inverse(latent), inverse(context)])[None]

    def share(tokens):
        quarter = tokens.shape[0] // tp
        own = lax.dynamic_slice_in_dim(tokens, at_tp * quarter, quarter, 0)
        return own.reshape(quarter, sp, inner).transpose(1, 0, 2)

    terms_all, latent_all, context_all, scales_all, shift_all = relay(
        "sp",
        "tp",
        1,
        (terms, False, True, None),
        (share(latent), True, True, None),
        (share(context), True, True, None),
        (scales, False, False, None),
        (decay_shift.T[:, None, :], True, False, None),
    )
    modulation = jnp.sum(terms_all, axis=0).transpose(1, 0, 2).reshape(terms.shape[0], model)
    own_mod = lax.dynamic_slice_in_dim(modulation, at_sp * inner, inner, 1)
    own_gain = lax.dynamic_slice_in_dim(norm_gain, at_sp * inner, inner, 0)
    raw_latent = latent_all.reshape(sp * rows, inner)
    raw_context = context_all.reshape(sp * context_rows, inner)

    def tokens_of(raw, inverses, shift_row, scale_row):
        normalized = raw.astype(jnp.float32) * inverses.reshape(-1, 1)
        return (normalized * own_gain * (1.0 + scale_row) + shift_row).astype(jnp.bfloat16)

    h_latent = tokens_of(raw_latent, scales_all[:, 0, :rows], own_mod[0], own_mod[1])
    h_context = tokens_of(raw_context, scales_all[:, 0, rows:], own_mod[3], own_mod[4])
    h_all = jnp.concatenate([h_latent, h_context], axis=0)
    weights = jnp.concatenate(
        [
            w_query.reshape(inner, heads, DK),
            w_key.reshape(inner, heads, DK),
            w_value.reshape(inner, heads, DV),
        ],
        axis=2,
    ).transpose(1, 0, 2)
    partial = jnp.einsum(
        "tk,hkc->htc", h_all, weights, preferred_element_type=jnp.float32
    ).astype(jnp.bfloat16)

    def my_rows(tokens):
        cut = tokens.reshape(sp, tp, -1, inner)
        return lax.dynamic_index_in_dim(cut, at_tp, 1, False).reshape(-1, inner)

    rank_rows = jnp.concatenate([my_rows(h_latent), my_rows(h_context)], axis=0)
    rank_partial = jnp.dot(
        rank_rows,
        jnp.concatenate([w_rank[0], w_rank[1]], axis=1),
        preferred_element_type=jnp.float32,
    ).astype(jnp.bfloat16)
    rank_all, partial_all = relay(
        "sp", "tp", 3, (rank_partial, False, True, None), (partial, True, False, None)
    )
    rank_full = jnp.sum(rank_all.astype(jnp.float32), axis=0).astype(jnp.bfloat16)
    width = rank_full.shape[-1]
    cut = rank_rows.shape[0] - sp * context_rows // tp

    def in_order(tensor):
        return tensor.reshape(tp, sp, -1, width).transpose(1, 0, 2, 3).reshape(-1, width)

    ranks = jnp.concatenate([in_order(rank_full[:, :cut]), in_order(rank_full[:, cut:])], axis=0)
    joined = jnp.sum(partial_all.astype(jnp.float32), axis=0).astype(jnp.bfloat16)
    own_decay = lax.dynamic_slice_in_dim(w_decay, at_sp * DK, DK, 2)
    own_bias = lax.dynamic_slice_in_dim(decay_bias, at_sp * DK, DK, 1)
    half = width // 2
    fwd = log_decay(ranks[:, :half], own_decay[0], own_bias[0])
    bwd = log_decay(ranks[:, half:], own_decay[1], own_bias[1])
    span = sp * rows
    shift_rows = shift_all.reshape(span, 1)
    normed = mix(
        joined[:span, :DK],
        joined[:span, DK : 2 * DK],
        joined[:span, 2 * DK :],
        fwd[:span] + shift_rows,
        bwd[:span] + shift_rows,
        joined[span:, DK : 2 * DK],
        joined[span:, 2 * DK :],
        fwd[span:],
        bwd[span:],
        lax.dynamic_slice_in_dim(out_gain, at_sp * DV, DV, 0)[None],
    )
    (normed_all,) = exchange("sp", 5, (normed, False))
    part = jnp.einsum(
        "htc,hcd->td",
        normed_all,
        w_out.reshape(heads, DV, -1),
        preferred_element_type=jnp.float32,
    ).astype(jnp.bfloat16)
    columns = part.shape[1] // tp
    (part_all,) = exchange(
        "tp", 6, (part.reshape(span, tp, columns).transpose(1, 0, 2), True)
    )
    summed = jnp.sum(part_all.astype(jnp.float32), axis=0)
    gate = lax.dynamic_slice_in_dim(own_mod[2], at_tp * columns, columns, 0)
    residual = lax.dynamic_slice_in_dim(raw_latent, at_tp * columns, columns, 1)
    slab = (residual.astype(jnp.float32) + gate * summed).astype(jnp.bfloat16)
    (whole_rows,) = relay("sp", "tp", 7, (slab.reshape(sp, rows, columns), True, True, columns))
    return whole_rows


def chosen(mesh, *arrays):
    sizes = dict(mesh.shape)
    heads = arrays[6].shape[1]
    one_head_each = heads == DK * sizes["sp"] * sizes["tp"]
    return local_heads if one_head_each else local


def solution(mesh):
    return lambda *arrays: jax.shard_map(
        chosen(mesh, *arrays),
        mesh=mesh,
        in_specs=(
            P(("grp", "sp"), None),
            P(("grp", "sp"), None),
            P(("grp", "sp")),
            P(("grp", "sp")),
            P(None, "sp", "tp"),
            P(),
            P("sp", "tp"),
            P("sp", "tp"),
            P("sp", "tp"),
            P(None, "sp", None),
            P(None, None, "tp"),
            P(None, "tp"),
            P(("grp", "sp"), "tp"),
            P("tp"),
            P("tp", "sp"),
        ),
        out_specs=P(("grp", "sp"), None),
        check_vma=False,
    )(*arrays)
```

```python
import functools

import jax
import jax.numpy as jnp
from jax import lax
from jax.experimental import pallas as pl
from jax.experimental.pallas import tpu as pltpu
from jax.sharding import PartitionSpec as P

DK = 64
DV = 128
BLOCK = 64


eps = 1e-06
normalizer = 16.0
precise = lax.Precision.HIGHEST


def carried_in(array, axis, join, neutral, backward):
    count = lax.axis_size(axis)
    place = lax.axis_index(axis)
    ahead = count - 1 - place if backward else place
    gathered = jax.tree.map(
        lambda a, kind: lax.all_gather(a.astype(kind), axis),
        array,
        jax.tree.map(lambda a: jnp.bfloat16 if a.dtype == jnp.float32 else a.dtype, array),
    )
    state = jax.tree.map(lambda a, e: jnp.zeros_like(a) + jnp.asarray(e, a.dtype), array, neutral)

    def one(turn, state):
        source = count - 1 - turn if backward else turn
        return join(
            state,
            jax.tree.map(
                lambda a, own: lax.dynamic_index_in_dim(a, source, 0, False).astype(own.dtype),
                gathered,
                array,
            ),
        )

    return lax.fori_loop(0, ahead, one, state)


def rounded(tensor):
    return lax.optimization_barrier(tensor.astype(jnp.bfloat16))


def modulated(tokens, norm_gain, shift_row, scale_row):
    widened = tokens.astype(jnp.float32)
    normalized = widened * lax.rsqrt(jnp.mean(widened * widened, axis=-1, keepdims=True) + eps)
    return (normalized * norm_gain * (1.0 + scale_row) + shift_row).astype(jnp.bfloat16)


def project(tokens, weight):
    return rounded(jnp.dot(tokens, weight, preferred_element_type=jnp.float32))


def log_decay(rank_rows, weight, bias):
    return (
        jax.nn.log_sigmoid(jnp.dot(rank_rows, weight, preferred_element_type=jnp.float32) + bias)
        / normalizer
    )


def by_heads(tensor, width):
    return tensor.astype(jnp.float32).reshape(tensor.shape[0], -1, width)


def context_state(key_rows, value_rows, decays, forward):
    running = jnp.cumsum(decays, axis=0)
    if forward:
        factor = jnp.exp(running[-1] - running)
    else:
        factor = jnp.exp(running - decays)
    return jnp.einsum("thd,the->hde", key_rows * factor, value_rows, precision=precise)


def chained(earlier, later):
    return (earlier[0] + later[0], jnp.exp(later[0])[:, :, None] * earlier[1] + later[1])


def segment_chain(queries, key_rows, value_rows, decays):
    length, head_count, width = queries.shape
    blocks = length // BLOCK
    lower_mask = jnp.tril(jnp.ones((BLOCK, BLOCK), dtype=bool))

    def in_blocks(tensor):
        return tensor.reshape(blocks, BLOCK, head_count, tensor.shape[-1])

    def advance(carry, inputs):
        carry_state, offset = carry
        query_block, key_block, value_block, decay_block = inputs
        running = jnp.cumsum(decay_block, axis=0)
        carried = jnp.einsum(
            "chd,hde->che", query_block * jnp.exp(running), carry_state, precision=precise
        )
        flat_running = running.reshape(BLOCK, head_count * width)
        relative = jnp.where(
            lower_mask[:, :, None], flat_running[:, None] - flat_running[None, :], -jnp.inf
        )
        products = (
            jnp.exp(relative) * query_block.reshape(BLOCK, 1, -1) * key_block.reshape(1, BLOCK, -1)
        )
        scores = products.reshape(BLOCK, BLOCK, head_count, width).sum(axis=-1)
        within = jnp.einsum("ijh,jhe->ihe", scores, value_block, precision=precise)
        block_total = running[-1]
        carry_state = jnp.exp(block_total)[:, :, None] * carry_state + jnp.einsum(
            "chd,che->hde",
            key_block * jnp.exp(block_total - running),
            value_block,
            precision=precise,
        )
        lifted = query_block * jnp.exp(offset + running)
        return ((carry_state, offset + block_total), (carried + within, lifted))

    initial = (
        jnp.zeros((head_count, width, value_rows.shape[-1]), jnp.float32),
        jnp.zeros((head_count, width), jnp.float32),
    )
    (final_state, totals), (outputs, lifted) = lax.scan(
        advance,
        initial,
        (in_blocks(queries), in_blocks(key_rows), in_blocks(value_rows), in_blocks(decays)),
    )
    return (
        outputs.reshape(length, head_count, -1),
        lifted.reshape(length, head_count, width),
        (totals, final_state),
    )


def local(
    latent,
    context,
    cond_latent,
    cond_context,
    mod_weight,
    norm_gain,
    w_query,
    w_key,
    w_value,
    w_rank,
    w_decay,
    decay_bias,
    decay_shift,
    out_gain,
    w_out,
):
    silu_latent = jax.nn.silu(cond_latent).astype(jnp.bfloat16)
    silu_context = jax.nn.silu(cond_context).astype(jnp.bfloat16)
    term_latent = jnp.einsum(
        "d,rdc->rc", silu_latent, mod_weight, preferred_element_type=jnp.float32
    )
    term_context = jnp.einsum(
        "d,rdc->rc", silu_context, mod_weight[:2], preferred_element_type=jnp.float32
    )
    terms = jnp.concatenate([term_latent, term_context], axis=0)
    summed_terms = lax.psum(terms, "sp")
    modulation = lax.all_gather(summed_terms, "tp", axis=1, tiled=True)
    query_all, key_all, value_all, rank_all, output_all, context_rows = (
        lax.all_gather(w_query, "sp", axis=0, tiled=True),
        lax.all_gather(w_key, "sp", axis=0, tiled=True),
        lax.all_gather(w_value, "sp", axis=0, tiled=True),
        lax.all_gather(w_rank, "sp", axis=1, tiled=True),
        lax.all_gather(w_out, "sp", axis=1, tiled=True),
        lax.all_gather(context, "sp", axis=0, tiled=True),
    )
    h_latent = modulated(latent, norm_gain, modulation[0], modulation[1])
    h_context = modulated(context_rows, norm_gain, modulation[3], modulation[4])
    queries = by_heads(project(h_latent, query_all), DK)
    key_rows = by_heads(project(h_latent, key_all), DK)
    value_rows = by_heads(project(h_latent, value_all), DV)
    shift_rows = decay_shift[:, :, None]
    log_fwd = (
        by_heads(log_decay(project(h_latent, rank_all[0]), w_decay[0], decay_bias[0]), DK)
        + shift_rows
    )
    log_bwd = (
        by_heads(log_decay(project(h_latent, rank_all[1]), w_decay[1], decay_bias[1]), DK)
        + shift_rows
    )
    context_keys = by_heads(project(h_context, key_all), DK)
    context_values = by_heads(project(h_context, value_all), DV)
    context_fwd = by_heads(
        log_decay(project(h_context, rank_all[0]), w_decay[0], decay_bias[0]), DK
    )
    context_bwd = by_heads(
        log_decay(project(h_context, rank_all[1]), w_decay[1], decay_bias[1]), DK
    )
    own_fwd = (
        jnp.sum(context_fwd, axis=0),
        context_state(context_keys, context_values, context_fwd, True),
    )
    own_bwd = (
        jnp.sum(context_bwd, axis=0),
        context_state(context_keys, context_values, context_bwd, False),
    )
    out_fwd, lift_fwd, pair_fwd = segment_chain(queries, key_rows, value_rows, log_fwd)
    flipped_out, flipped_lift, pair_bwd = segment_chain(
        jnp.flip(queries, 0), jnp.flip(key_rows, 0), jnp.flip(value_rows, 0), jnp.flip(log_bwd, 0)
    )
    out_bwd = jnp.flip(flipped_out, 0)
    lift_bwd = jnp.flip(flipped_lift, 0)
    zero_pair = (jnp.zeros_like(pair_fwd[0]), jnp.zeros_like(pair_fwd[1]))
    before = carried_in(pair_fwd, "sp", chained, zero_pair, False)
    after = carried_in(pair_bwd, "sp", chained, zero_pair, True)
    start_fwd = own_fwd[1]
    start_bwd = own_bwd[1]
    entry_forward = chained((zero_pair[0], start_fwd), before)[1]
    entry_bwd = chained((zero_pair[0], start_bwd), after)[1]
    combined = (
        out_fwd
        + out_bwd
        + jnp.einsum("thd,hde->the", lift_fwd, entry_forward, precision=precise)
        + jnp.einsum("thd,hde->the", lift_bwd, entry_bwd, precision=precise)
    )
    combined = combined * lax.rsqrt(jnp.mean(combined * combined, axis=-1, keepdims=True) + eps)
    normed = (combined.reshape(combined.shape[0], -1) * out_gain).astype(jnp.bfloat16)
    partial_out = jnp.dot(normed, output_all, preferred_element_type=jnp.float32)
    summed = lax.psum(partial_out.astype(jnp.bfloat16), "tp").astype(jnp.float32)
    return (latent.astype(jnp.float32) + modulation[2] * summed).astype(jnp.bfloat16)


MESH = pl.DeviceIdType.MESH
SUB = 16


def exchange_kernel(axis, count, sends, *refs):
    total = len(sends)
    sources, targets = refs[:total], refs[total : 2 * total]
    send_sem, recv_sem, own_sem = refs[2 * total :]
    me = lax.axis_index(axis)
    barrier = pltpu.get_barrier_semaphore()
    for step in range(1, count):
        pl.semaphore_signal(
            barrier, inc=1, device_id={axis: lax.rem(me + step, count)}, device_id_type=MESH
        )
    pl.semaphore_wait(barrier, count - 1)

    def columns(ref, index, width):
        return ref.at[:, pl.ds(pl.multiple_of(index * width, width), width)]

    def taken(item, peer):
        if not sends[item]:
            return sources[item]
        return columns(sources[item], peer, targets[item].shape[2])

    def placed(item):
        if sends[item]:
            return targets[item].at[me]
        return columns(targets[item], me, sources[item].shape[1])

    copies = []
    for item in range(total):
        for step in range(1, count):
            peer = lax.rem(me + step, count)
            copy = pltpu.make_async_remote_copy(
                src_ref=taken(item, peer),
                dst_ref=placed(item),
                send_sem=send_sem.at[item, step - 1],
                recv_sem=recv_sem.at[item, step - 1],
                device_id={axis: peer},
                device_id_type=MESH,
            )
            copy.start()
            copies.append(copy)
    for item in range(total):
        copy = pltpu.make_async_copy(
            taken(item, me),
            placed(item),
            own_sem.at[item],
        )
        copy.start()
        copies.append(copy)
    for copy in copies:
        copy.wait()


def exchange(axis, collective, *items):
    count = lax.axis_size(axis)
    sends = tuple(scatter for _, scatter in items)
    arrays = [array for array, _ in items]
    shapes = [
        jax.ShapeDtypeStruct(
            (count, a.shape[0], a.shape[1] // count) if s else (a.shape[0], count * a.shape[1]),
            a.dtype,
        )
        for a, s in items
    ]
    return pl.pallas_call(
        functools.partial(exchange_kernel, axis, count, sends),
        out_shape=shapes,
        in_specs=[pl.BlockSpec(memory_space=pltpu.VMEM)] * len(items),
        out_specs=[pl.BlockSpec(memory_space=pltpu.VMEM)] * len(items),
        scratch_shapes=[
            pltpu.SemaphoreType.DMA((len(items), count - 1)),
            pltpu.SemaphoreType.DMA((len(items), count - 1)),
            pltpu.SemaphoreType.DMA((len(items),)),
        ],
        compiler_params=pltpu.CompilerParams(collective_id=collective, has_side_effects=True),
        name=f"exchange_{collective}",
    )(*arrays)


def relay_kernel(across, along, items, meanwhile, *refs):
    total = len(items)
    sources, targets = refs[:total], refs[total : 2 * total]
    own_sem, far_send, far_recv, near_send, near_recv, pass_send, pass_recv = refs[2 * total :]
    far, near = lax.axis_size(across), lax.axis_size(along)
    here, mine = lax.axis_index(across), lax.axis_index(along)
    pairs = near // 2
    partner = mine + 1 - 2 * lax.rem(mine, 2)
    barrier = pltpu.get_barrier_semaphore()
    for step in range(1, far):
        pl.semaphore_signal(
            barrier, inc=1, device_id={across: lax.rem(here + step, far)}, device_id_type=MESH
        )
    pl.semaphore_signal(barrier, inc=1, device_id={along: partner}, device_id_type=MESH)
    for step in range(1, pairs):
        pl.semaphore_signal(
            barrier, inc=1, device_id={along: lax.rem(mine + 2 * step, near)}, device_id_type=MESH
        )
    pl.semaphore_wait(barrier, far - 1 + pairs)

    def view(item, source, holder):
        scatter, forward, block = items[item]
        target = targets[item]
        if not forward:
            return target.at[source]
        if block is None:
            return target.at[source, holder]
        start = pl.multiple_of((source * near + holder) * block, block)
        return target.at[:, pl.ds(start, block)]

    def taken(item, peer):
        return sources[item].at[peer] if items[item][0] else sources[item]

    first, sent, arrive = {}, [], []
    for item in range(total):
        copy = pltpu.make_async_copy(taken(item, here), view(item, here, mine), own_sem.at[item])
        copy.start()
        first[item, 0] = copy
        for step in range(1, far):
            peer = lax.rem(here + step, far)
            copy = pltpu.make_async_remote_copy(
                src_ref=taken(item, peer),
                dst_ref=view(item, here, mine),
                send_sem=far_send.at[item, step],
                recv_sem=far_recv.at[item, step],
                device_id={across: peer},
                device_id_type=MESH,
            )
            copy.start()
            first[item, step] = copy
            sent.append(copy)

    if meanwhile is not None:
        meanwhile()

    def hand(item, step, block, slot, sends, recvs, peer):
        copy = pltpu.make_async_remote_copy(
            src_ref=block,
            dst_ref=block,
            send_sem=sends.at[item, step, slot],
            recv_sem=recvs.at[item, step, slot],
            device_id={along: peer},
            device_id_type=MESH,
        )
        copy.start()
        sent.append(copy)
        return copy

    crossed = []

    def pass_on():
        for item, step, source, slot, copy in crossed:
            copy.wait_recv()
            holder = lax.rem(mine + near - 2 * slot, near)
            block = view(item, source, holder)
            arrive.append(hand(item, step, block, slot, pass_send, pass_recv, partner))
        crossed.clear()

    for step in range(far):
        source = lax.rem(here - step + far, far)
        fresh = []
        for item in range(total):
            if not items[item][1]:
                continue
            if step:
                first[item, step].wait_recv()
            else:
                first[item, step].wait()
            block = view(item, source, mine)
            for slot in range(1, pairs):
                peer = lax.rem(mine + 2 * slot, near)
                copy = hand(item, step, block, slot, near_send, near_recv, peer)
                fresh.append((item, step, source, slot, copy))
            arrive.append(hand(item, step, block, 0, near_send, near_recv, partner))
        pass_on()
        crossed.extend(fresh)
    pass_on()
    for item in range(total):
        if not items[item][1]:
            first[item, 0].wait()
            for step in range(1, far):
                first[item, step].wait_recv()
    for copy in arrive:
        copy.wait_recv()
    for copy in sent:
        copy.wait_send()


def relay(across, along, collective, *items):
    far, near = lax.axis_size(across), lax.axis_size(along)
    shapes = []
    for array, scatter, forward, block in items:
        shape = array.shape[1:] if scatter else array.shape
        if block is not None:
            full = (shape[0], far * near * block)
        elif forward:
            full = (far, near) + shape
        else:
            full = (far,) + shape
        shapes.append(jax.ShapeDtypeStruct(full, array.dtype))
    dma = pltpu.SemaphoreType.DMA
    count, pairs = len(items), near // 2
    return pl.pallas_call(
        functools.partial(relay_kernel, across, along, tuple(i[1:] for i in items), None),
        out_shape=shapes,
        in_specs=[pl.BlockSpec(memory_space=pltpu.VMEM)] * count,
        out_specs=[pl.BlockSpec(memory_space=pltpu.VMEM)] * count,
        scratch_shapes=[dma((count,)), dma((count, far)), dma((count, far))]
        + [dma((count, far, pairs))] * 4,
        compiler_params=pltpu.CompilerParams(collective_id=collective, has_side_effects=True),
        name=f"relay_{collective}",
    )(*[item[0] for item in items])


def join_kernel(across, along, rank_ref, part_ref, rank_out, joined_ref, *scratch):
    relay_sems = scratch[:7]
    buffers, sends, recvs = scratch[7:11], scratch[11], scratch[12]
    came, gone = buffers[:2], buffers[2:]
    count = lax.axis_size(across)
    me = lax.axis_index(across)
    rows = joined_ref.shape[0]
    tiles = rows // BLOCK

    def copy(side, owner, source):
        return pltpu.make_async_remote_copy(
            src_ref=source,
            dst_ref=came[side].at[owner],
            send_sem=sends.at[side, owner],
            recv_sem=recvs.at[side, owner],
            device_id={across: lax.rem(me + (1 if side == 0 else count - 1), count)},
            device_id_type=MESH,
        )

    def owners(side):
        return range(count - 1, 0, -1) if side == 0 else range(count - 1)

    def first(side):
        return me == (0 if side == 0 else count - 1)

    def between(side, owner):
        return (me > 0) & (me < owner) if side == 0 else (me < count - 1) & (me > owner)

    def ends():
        for side in range(2):

            @pl.when(first(side))
            def _():
                for owner in owners(side):
                    copy(side, owner, part_ref.at[owner]).start()

    relay_kernel(across, along, ((False, True, None),), ends, rank_ref, rank_out, *relay_sems)

    def step(side, owner):
        @pl.when(between(side, owner))
        def _():
            copy(side, owner, gone[side].at[owner]).wait_recv()

            def add(tile, carry):
                span = pl.ds(pl.multiple_of(tile * BLOCK, BLOCK), BLOCK)
                total = part_ref[owner, span, :].astype(jnp.float32) + came[side][
                    owner, span, :
                ].astype(jnp.float32)
                gone[side][owner, span, :] = total.astype(jnp.bfloat16)
                return carry

            lax.fori_loop(0, tiles, add, 0)
            copy(side, owner, gone[side].at[owner]).start()

    def all_steps(sides):
        for turn in range(count - 1):
            for side in sides:
                step(side, owners(side)[turn])

    lower = me < count // 2

    @pl.when(lower)
    def _():
        all_steps((0, 1))

    @pl.when(jnp.logical_not(lower))
    def _():
        all_steps((1, 0))

    def collect(use):
        for side in range(2):
            if use[side]:
                copy(side, me, gone[side].at[me]).wait_recv()

        def add(tile, carry):
            span = pl.ds(pl.multiple_of(tile * BLOCK, BLOCK), BLOCK)
            total = part_ref[me, span, :].astype(jnp.float32)
            for side in range(2):
                if use[side]:
                    total = total + came[side][me, span, :].astype(jnp.float32)
            joined_ref[span, :] = total.astype(jnp.bfloat16)
            return carry

        lax.fori_loop(0, tiles, add, 0)

    @pl.when(first(0))
    def _():
        collect((False, True))

    @pl.when(first(1))
    def _():
        collect((True, False))

    @pl.when((me > 0) & (me < count - 1))
    def _():
        collect((True, True))

    for side in range(2):
        for owner in owners(side):

            @pl.when(between(side, owner))
            def _():
                copy(side, owner, gone[side].at[owner]).wait_send()

            @pl.when(first(side))
            def _():
                copy(side, owner, part_ref.at[owner]).wait_send()


def join(across, along, collective, rank, partial):
    far, near = lax.axis_size(across), lax.axis_size(along)
    dma = pltpu.SemaphoreType.DMA
    return pl.pallas_call(
        functools.partial(join_kernel, across, along),
        out_shape=[
            jax.ShapeDtypeStruct((far, near) + rank.shape, rank.dtype),
            jax.ShapeDtypeStruct(partial.shape[1:], partial.dtype),
        ],
        in_specs=[pl.BlockSpec(memory_space=pltpu.VMEM)] * 2,
        out_specs=[pl.BlockSpec(memory_space=pltpu.VMEM)] * 2,
        scratch_shapes=[dma((1,)), dma((1, far)), dma((1, far))]
        + [dma((1, far, near // 2))] * 4
        + [pltpu.VMEM(partial.shape, partial.dtype)] * 4
        + [dma((2, far)), dma((2, far))],
        compiler_params=pltpu.CompilerParams(collective_id=collective, has_side_effects=True),
        name="join",
    )(rank, partial)


def narrow_dot(left, right, dims):
    return lax.dot_general(
        left.astype(jnp.bfloat16),
        right.astype(jnp.bfloat16),
        (dims, ((), ())),
        preferred_element_type=jnp.float32,
    )


def mix_kernel(q_ref, k_ref, v_ref, f_ref, b_ref, ck_ref, cv_ref, cf_ref, cb_ref, gain_ref, o_ref, later_ref):
    length, width = q_ref.shape
    depth = v_ref.shape[1]
    row = lax.broadcasted_iota(jnp.int32, (BLOCK, BLOCK), 0)
    column = lax.broadcasted_iota(jnp.int32, (BLOCK, BLOCK), 1)
    lower = jnp.where(row >= column, 1.0, 0.0).astype(jnp.float32)
    upper = jnp.where(row <= column, 1.0, 0.0).astype(jnp.float32)
    key_row = lax.broadcasted_iota(jnp.int32, (BLOCK, width), 0)

    def sums(ones, decays):
        return jnp.dot(ones, decays, precision=precise, preferred_element_type=jnp.float32)

    def step(state, keys, values, running, block_total):
        return state * jnp.exp(block_total) + narrow_dot(
            values, keys * jnp.exp(block_total - running), ((0,), (0,))
        )

    def at(ref, index):
        return ref[pl.ds(pl.multiple_of(index * BLOCK, BLOCK), BLOCK), :].astype(jnp.float32)

    zero = jnp.zeros((depth, width), jnp.float32)
    context_blocks = ck_ref.shape[0] // BLOCK
    blocks = length // BLOCK

    def context_forward(index, state):
        running = sums(lower, at(cf_ref, index))
        return step(state, at(ck_ref, index), at(cv_ref, index), running, running[BLOCK - 1 :])

    def context_backward(turn, state):
        index = context_blocks - 1 - turn
        running = sums(upper, at(cb_ref, index))
        return step(state, at(ck_ref, index), at(cv_ref, index), running, running[:1])

    start_fwd = lax.fori_loop(0, context_blocks, context_forward, zero)
    start_bwd = lax.fori_loop(0, context_blocks, context_backward, zero)

    def backward(turn, state):
        index = blocks - 1 - turn
        later_ref[index] = state
        running = sums(upper, at(b_ref, index))
        return step(state, at(k_ref, index), at(v_ref, index), running, running[:1])

    lax.fori_loop(0, blocks, backward, start_bwd)

    def forward(index, state):
        queries, keys, values = at(q_ref, index), at(k_ref, index), at(v_ref, index)
        ahead = sums(lower, at(f_ref, index))
        behind = sums(upper, at(b_ref, index))
        pieces = []
        for sub in range(BLOCK // SUB):
            low, high = sub * SUB, (sub + 1) * SUB
            own = slice(low, high)
            left, right = [], []
            if low:
                edge = ahead[low - 1 : low]
                left.append(queries[own] * jnp.exp(ahead[own] - edge))
                right.append(
                    jnp.where(key_row < low, keys * jnp.exp(jnp.minimum(edge - ahead, 0.0)), 0.0)
                )
            if high < BLOCK:
                edge = behind[high : high + 1]
                left.append(queries[own] * jnp.exp(behind[own] - edge))
                right.append(
                    jnp.where(key_row >= high, keys * jnp.exp(jnp.minimum(edge - behind, 0.0)), 0.0)
                )
            piece = narrow_dot(left[0], right[0], ((1,), (1,)))
            for one, other in zip(left[1:], right[1:]):
                piece = piece + narrow_dot(one, other, ((1,), (1,)))
            pieces.append(piece)
        scores = jnp.concatenate(pieces, axis=0)

        def cut(tensor):
            return tensor.reshape(BLOCK // SUB, SUB, width)

        q3, k3, a3, b3 = cut(queries), cut(keys), cut(ahead), cut(behind)
        inner = lax.broadcasted_iota(jnp.int32, q3.shape, 1)
        for other in range(SUB):
            one = slice(other, other + 1)
            relative = jnp.where(inner >= other, a3 - a3[:, one], b3 - b3[:, one])
            product = jnp.exp(relative) * q3 * k3[:, one]
            product = jnp.where(inner == other, 2.0 * product, product)
            near = jnp.sum(product.reshape(BLOCK, width), axis=-1, keepdims=True)
            scores = scores + jnp.where(column == (row // SUB) * SUB + other, near, 0.0)
        output = (
            narrow_dot(scores, values, ((1,), (0,)))
            + narrow_dot(queries * jnp.exp(ahead), state, ((1,), (1,)))
            + narrow_dot(queries * jnp.exp(behind), later_ref[index], ((1,), (1,)))
        )
        output = output * lax.rsqrt(jnp.mean(output * output, axis=-1, keepdims=True) + eps)
        o_ref[pl.ds(pl.multiple_of(index * BLOCK, BLOCK), BLOCK), :] = (
            output * gain_ref[...]
        ).astype(o_ref.dtype)
        return step(state, keys, values, ahead, ahead[BLOCK - 1 :])

    lax.fori_loop(0, blocks, forward, start_fwd)


def mix(queries, key_rows, value_rows, log_fwd, log_bwd, keys, values, fwd, bwd, gain):
    length, width = queries.shape
    depth = value_rows.shape[1]
    return pl.pallas_call(
        mix_kernel,
        out_shape=jax.ShapeDtypeStruct((length, depth), jnp.bfloat16),
        in_specs=[pl.BlockSpec(memory_space=pltpu.VMEM)] * 10,
        out_specs=pl.BlockSpec(memory_space=pltpu.VMEM),
        scratch_shapes=[pltpu.VMEM((length // BLOCK, depth, width), jnp.float32)],
        name="mix",
    )(queries, key_rows, value_rows, log_fwd, log_bwd, keys, values, fwd, bwd, gain)


def local_heads(
    latent,
    context,
    cond_latent,
    cond_context,
    mod_weight,
    norm_gain,
    w_query,
    w_key,
    w_value,
    w_rank,
    w_decay,
    decay_bias,
    decay_shift,
    out_gain,
    w_out,
):
    sp, tp = lax.axis_size("sp"), lax.axis_size("tp")
    at_sp, at_tp = lax.axis_index("sp"), lax.axis_index("tp")
    rows, model = latent.shape
    context_rows = context.shape[0]
    inner = model // sp
    heads = w_query.shape[1] // DK
    silu_latent = jax.nn.silu(cond_latent).astype(jnp.bfloat16)
    silu_context = jax.nn.silu(cond_context).astype(jnp.bfloat16)
    term_latent = jnp.einsum(
        "d,rdc->rc", silu_latent, mod_weight, preferred_element_type=jnp.float32
    )
    term_context = jnp.einsum(
        "d,rdc->rc", silu_context, mod_weight[:2], preferred_element_type=jnp.float32
    )
    terms = jnp.concatenate([term_latent, term_context], axis=0)

    def inverse(tokens):
        widened = tokens.astype(jnp.float32)
        return lax.rsqrt(jnp.mean(widened * widened, axis=-1) + eps)

    scales = jnp.concatenate([inverse(latent), inverse(context)])[None]

    def share(tokens):
        quarter = tokens.shape[0] // tp
        own = lax.dynamic_slice_in_dim(tokens, at_tp * quarter, quarter, 0)
        return own.reshape(quarter, sp, inner).transpose(1, 0, 2)

    terms_all, latent_all, context_all, scales_all, shift_all = relay(
        "sp",
        "tp",
        1,
        (terms, False, True, None),
        (share(latent), True, True, None),
        (share(context), True, True, None),
        (scales, False, False, None),
        (decay_shift.T[:, None, :], True, False, None),
    )
    modulation = jnp.sum(terms_all, axis=0).transpose(1, 0, 2).reshape(terms.shape[0], model)
    own_mod = lax.dynamic_slice_in_dim(modulation, at_sp * inner, inner, 1)
    own_gain = lax.dynamic_slice_in_dim(norm_gain, at_sp * inner, inner, 0)
    raw_latent = latent_all.reshape(sp * rows, inner)
    raw_context = context_all.reshape(sp * context_rows, inner)

    def tokens_of(raw, inverses, shift_row, scale_row):
        normalized = raw.astype(jnp.float32) * inverses.reshape(-1, 1)
        return (normalized * own_gain * (1.0 + scale_row) + shift_row).astype(jnp.bfloat16)

    h_latent = tokens_of(raw_latent, scales_all[:, 0, :rows], own_mod[0], own_mod[1])
    h_context = tokens_of(raw_context, scales_all[:, 0, rows:], own_mod[3], own_mod[4])
    h_all = jnp.concatenate([h_latent, h_context], axis=0)
    weights = jnp.concatenate(
        [
            w_query.reshape(inner, heads, DK),
            w_key.reshape(inner, heads, DK),
            w_value.reshape(inner, heads, DV),
        ],
        axis=2,
    ).transpose(1, 0, 2)
    partial = jnp.einsum(
        "tk,hkc->htc", h_all, weights, preferred_element_type=jnp.float32
    ).astype(jnp.bfloat16)

    def my_rows(tokens):
        cut = tokens.reshape(sp, tp, -1, inner)
        return lax.dynamic_index_in_dim(cut, at_tp, 1, False).reshape(-1, inner)

    rank_rows = jnp.concatenate([my_rows(h_latent), my_rows(h_context)], axis=0)
    rank_partial = jnp.dot(
        rank_rows,
        jnp.concatenate([w_rank[0], w_rank[1]], axis=1),
        preferred_element_type=jnp.float32,
    ).astype(jnp.bfloat16)
    rank_all, joined = join("sp", "tp", 3, rank_partial, partial)
    rank_full = jnp.sum(rank_all.astype(jnp.float32), axis=0).astype(jnp.bfloat16)
    width = rank_full.shape[-1]
    cut = rank_rows.shape[0] - sp * context_rows // tp

    def in_order(tensor):
        return tensor.reshape(tp, sp, -1, width).transpose(1, 0, 2, 3).reshape(-1, width)

    ranks = jnp.concatenate([in_order(rank_full[:, :cut]), in_order(rank_full[:, cut:])], axis=0)
    own_decay = lax.dynamic_slice_in_dim(w_decay, at_sp * DK, DK, 2)
    own_bias = lax.dynamic_slice_in_dim(decay_bias, at_sp * DK, DK, 1)
    half = width // 2
    fwd = log_decay(ranks[:, :half], own_decay[0], own_bias[0])
    bwd = log_decay(ranks[:, half:], own_decay[1], own_bias[1])
    span = sp * rows
    shift_rows = shift_all.reshape(span, 1)
    normed = mix(
        joined[:span, :DK],
        joined[:span, DK : 2 * DK],
        joined[:span, 2 * DK :],
        fwd[:span] + shift_rows,
        bwd[:span] + shift_rows,
        joined[span:, DK : 2 * DK],
        joined[span:, 2 * DK :],
        fwd[span:],
        bwd[span:],
        lax.dynamic_slice_in_dim(out_gain, at_sp * DV, DV, 0)[None],
    )
    (normed_all,) = exchange("sp", 5, (normed, False))
    part = jnp.dot(normed_all, w_out, preferred_element_type=jnp.float32).astype(jnp.bfloat16)
    columns = part.shape[1] // tp
    (part_all,) = exchange("tp", 6, (part, True))
    summed = jnp.sum(part_all.astype(jnp.float32), axis=0)
    gate = lax.dynamic_slice_in_dim(own_mod[2], at_tp * columns, columns, 0)
    residual = lax.dynamic_slice_in_dim(raw_latent, at_tp * columns, columns, 1)
    slab = (residual.astype(jnp.float32) + gate * summed).astype(jnp.bfloat16)
    (whole_rows,) = relay("sp", "tp", 7, (slab.reshape(sp, rows, columns), True, True, columns))
    return whole_rows


def chosen(mesh, *arrays):
    sizes = dict(mesh.shape)
    heads = arrays[6].shape[1]
    one_head_each = heads == DK * sizes["sp"] * sizes["tp"]
    return local_heads if one_head_each else local


def solution(mesh):
    return lambda *arrays: jax.shard_map(
        chosen(mesh, *arrays),
        mesh=mesh,
        in_specs=(
            P(("grp", "sp"), None),
            P(("grp", "sp"), None),
            P(("grp", "sp")),
            P(("grp", "sp")),
            P(None, "sp", "tp"),
            P(),
            P("sp", "tp"),
            P("sp", "tp"),
            P("sp", "tp"),
            P(None, "sp", None),
            P(None, None, "tp"),
            P(None, "tp"),
            P(("grp", "sp"), "tp"),
            P("tp"),
            P("tp", "sp"),
        ),
        out_specs=P(("grp", "sp"), None),
        check_vma=False,
    )(*arrays)
```
